32 devices in a mesh: sp: 8 (over z, x), tp: 4 (over y, core).
Axes of the slice: x: 2, y: 2, z: 4, core: 2. Of those that a mesh axis runs over, the one named last changes fastest.
Arguments:
- queries: bfloat16 [4096, 512], P('sp', 'tp'), may hold values from -16 to 16
- key_heads: bfloat16 [4096, 512], P('sp', 'tp'), may hold values from -16 to 16
- value_heads: bfloat16 [4096, 512], P('sp', 'tp'), may hold values from -6 to 6
- head_gain: float32 [512], P('tp'), may hold values from 0.1 to 1.9
- residual: bfloat16 [4096, 2048], P(('sp', 'tp')), may hold values from -6 to 6
- out_weight: bfloat16 [512, 2048], replicated, may hold values from -0.25 to 0.25
- norm_gain: float32 [2048], replicated, may hold values from 0.1 to 1.9
- shared_gate: bfloat16 [2048, 512], replicated, may hold values from -0.125 to 0.125
- shared_up: bfloat16 [2048, 512], replicated, may hold values from -0.125 to 0.125
- shared_down: bfloat16 [512, 2048], replicated, may hold values from -0.25 to 0.25
- expert_gate: bfloat16 [64, 2048, 512], P(('sp', 'tp')), may hold values from -0.125 to 0.125
- expert_up: bfloat16 [64, 2048, 512], P(('sp', 'tp')), may hold values from -0.125 to 0.125
- expert_down: bfloat16 [64, 512, 2048], P(('sp', 'tp')), may hold values from -0.25 to 0.25
- routed_experts: int32 [4096, 4], P(('sp', 'tp')), may hold values from 0 to 63, all different within a row; in each aligned block of 128 rows (0 to 127, 128 to 255, ...) at most 12 rows name the same one
- route_weights: float32 [4096, 4], P(('sp', 'tp')), may hold values from 0.1 to 1.5
Outputs:
- layer_output: bfloat16 [4096, 2048], P(('sp', 'tp'))
The draws below stay inside these ranges and needn't reach their ends.
Inputs may be any that keep to these rules, and one draw needn't show every extreme that they name: `routed_experts`: each row names 4 different experts. Within the rows of one device (128 consecutive rows, aligned) no expert is named more than 12 times, and in every draw some expert is named exactly 12 times in some device's rows.
All inputs are finite; a program needn't handle non-finite values.
Results may differ from the reference program's by a relative error of at most 0.014.
Values may be sent and summed in bfloat16 or wider, within the bound.
No kernel may reach another device: no remote copies, remote signals or barrier semaphores. Data moves between devices by JAX's collectives and lax.ppermute only.
A program may use at most 128 MiB of HBM per device.

```python
import math
import jax
import jax.numpy as jnp
import numpy as np
from jax import lax

D = 2048
HEADS = 8
HEAD_DIM = 64
FFE = 512
SHARED_FF = 512
TOPK = 4
TOK_DEV = 128
TOK_SP = 512
TOKEN_COUNT = 4096
EXPERTS = 64
CAP = 12
N_SP = 8
N_TP = 4


def head_law(key):
    base_key = jax.random.fold_in(key, 11)
    direction_key, choice_key, quick_key, gentle_key = jax.random.split(base_key, 4)
    direction = jax.random.normal(direction_key, (HEADS, HEAD_DIM), jnp.float32)
    direction = direction / jnp.sqrt(jnp.sum(direction * direction, axis=1, keepdims=True))
    gentle_share = 0.5
    gentle = jax.random.uniform(choice_key, (HEADS,), jnp.float32) < gentle_share
    quick_rate = jnp.exp(jax.random.uniform(quick_key, (HEADS,), jnp.float32, math.log(3.3), math.log(4.6)))
    gentle_rate = math.log(TOKEN_COUNT) + jax.random.uniform(gentle_key, (HEADS,), jnp.float32, 0.0, 0.8)
    intensity = jnp.where(gentle, gentle_rate, quick_rate)
    return (direction, intensity)


def draw_queries(key, part):
    direction, intensity = head_law(key)
    noise = jnp.clip(jax.random.normal(jax.random.fold_in(key, 21), (TOKEN_COUNT, HEADS, HEAD_DIM), jnp.float32), -3.0, 3.0)
    lifted = jnp.sqrt(intensity * math.sqrt(HEAD_DIM))
    drawn = 0.5 * noise + lifted[None, :, None] * direction[None]
    return drawn.reshape(TOKEN_COUNT, HEADS * HEAD_DIM).astype(jnp.bfloat16)


def draw_key_heads(key, part):
    direction, intensity = head_law(key)
    jitter_random_key, shift_random_key, spike_random_key = jax.random.split(jax.random.fold_in(key, 31), 3)
    noise = jnp.clip(jax.random.normal(jitter_random_key, (TOKEN_COUNT, HEADS, HEAD_DIM), jnp.float32), -3.0, 3.0)
    shift_values = jax.random.uniform(shift_random_key, (TOKEN_COUNT // TOK_SP,), jnp.float32, -0.5, 0.5)
    shift_values = jnp.repeat(shift_values, TOK_SP)
    spike_amount = jax.random.uniform(spike_random_key, (TOKEN_COUNT,), jnp.float32) < 6.0 / TOKEN_COUNT
    lifted = jnp.sqrt(intensity * math.sqrt(HEAD_DIM))
    multiplier = jnp.where(spike_amount[:, None], 0.8 / intensity[None, :], 1.0 + shift_values[:, None] / intensity[None, :])
    drawn = 0.5 * noise - (lifted[None, :] * multiplier)[:, :, None] * direction[None]
    return drawn.reshape(TOKEN_COUNT, HEADS * HEAD_DIM).astype(jnp.bfloat16)


def levels(rng, extent, cuts, least, high):
    factor_of, own = 1.0, jax.random.fold_in(rng, 6)
    for position, shards_of in cuts:
        heights = jnp.exp(jax.random.uniform(jax.random.fold_in(own, position), (shards_of,), jnp.float32, least / len(cuts), high / len(cuts)))
        factor_of = factor_of * jnp.repeat(heights, extent[position] // shards_of).reshape([-1 if axis == position else 1 for axis in range(len(extent))])
    return factor_of


def assign_block(key, own, number, rows, number_of, top, reach, skew):
    order = jax.random.permutation(key, number_of)
    heavy_load, usual = load_shares(number_of, rows * top, reach, skew, True), load_shares(number_of, rows * top, reach, skew, False)
    places = jnp.arange(number_of)

    def named(tallies, turn):
        used = int((tallies > 0).sum())
        fixed = max(1, used // 4)
        shifted = fixed + (places - fixed + turn * (used - fixed)) % max(1, number_of - fixed)
        return jnp.zeros((number_of,), jnp.int32).at[order[jnp.where(places < fixed, places, shifted)]].set(jnp.asarray(tallies, jnp.int32))

    tallies = jnp.where(number % 4 == 0, named(heavy_load, number // 4), named(usual, number - number // 4 - 1))
    mixed = jax.random.permutation(jax.random.fold_in(own, 3), number_of)
    source_of, receiver = mixed[0:number_of // 2 * 2:2], mixed[1:number_of // 2 * 2:2]
    room = jnp.minimum(tallies[source_of] - 1, reach - tallies[receiver]) // 2
    room = jnp.where((source_of == order[0]) | (receiver == order[0]) | (tallies[receiver] == 0), 0, jnp.maximum(room, 0))
    shifted = jax.random.randint(jax.random.fold_in(own, 4), (number_of // 2,), 0, 1 << 20) % (room + 1)
    tallies = tallies.at[source_of].add(-shifted).at[receiver].add(shifted)
    labels = jnp.searchsorted(jnp.cumsum(tallies), jnp.arange(rows * top), side="right").astype(jnp.int32)
    grid = labels.reshape(top, rows).T
    grid = grid[jax.random.permutation(jax.random.fold_in(own, 1), rows)]
    turn = jax.random.randint(jax.random.fold_in(own, 2), (rows, 1), 0, top)
    return jnp.take_along_axis(grid, (jnp.arange(top)[None, :] + turn) % top, axis=1)


def load_shares(number_of, total, bound, lean, full):
    loads = [(1 << 20) // math.isqrt(rank ** lean) + 1 for rank in range(1, number_of + 1)]
    largest = bound if full else min(bound, max(-(-total // number_of), total * loads[0] // sum(loads)))
    least = 1 if total - largest >= number_of - 1 else 0
    holding, rest = [largest] + [least] * (number_of - 1), total - largest - least * (number_of - 1)
    while rest > 0:
        free = [i for i in range(1, number_of) if holding[i] < largest] or [i for i in range(1, number_of) if holding[i] < bound]
        pool, left = sum([loads[i] for i in free]), rest
        for i in free:
            extra = min(bound - holding[i], max(1, left * loads[i] // pool), rest)
            holding[i] = holding[i] + extra
            rest = rest - extra
    return np.array(holding)


def gaussian(rng, extent, scale, limit, cuts=(), kind=jnp.bfloat16):
    result = scale * jax.random.normal(rng, extent, jnp.float32)
    if cuts:
        result = result * levels(rng, extent, cuts, -0.22, 0.18)
    return jnp.clip(result, -limit, limit).astype(kind)


def setup_inputs(seed: int = 0) -> dict:
    key_of = jax.random.split(jax.random.key(seed), 16)
    queries = draw_queries(jax.random.fold_in(key_of[15], 71), 0)
    key_heads = draw_key_heads(jax.random.fold_in(key_of[15], 71), 0)
    value_heads = gaussian(key_of[2], (TOKEN_COUNT, HEADS * HEAD_DIM), 1.0, 6.0, ((0, 8), (1, 4)))
    head_gain = jnp.clip(1.0 + 0.18 * jax.random.normal(key_of[3], (HEADS * HEAD_DIM,), jnp.float32), 0.1, 1.9)
    residual = gaussian(key_of[4], (TOKEN_COUNT, D), 1.0, 6.0, ((0, 32),))
    out_weight = gaussian(key_of[5], (HEADS * HEAD_DIM, D), (HEADS * HEAD_DIM) ** -0.5, 0.25)
    norm_gain = jnp.clip(1.0 + 0.18 * jax.random.normal(key_of[6], (D,), jnp.float32), 0.1, 1.9)
    shared_gate = gaussian(key_of[7], (D, SHARED_FF), D ** -0.5, 0.125)
    shared_up = gaussian(key_of[8], (D, SHARED_FF), D ** -0.5, 0.125)
    shared_down = gaussian(key_of[9], (SHARED_FF, D), SHARED_FF ** -0.5, 0.25)
    expert_gate = gaussian(key_of[10], (EXPERTS, D, FFE), D ** -0.5, 0.125, ((0, 32),))
    expert_up = gaussian(key_of[11], (EXPERTS, D, FFE), D ** -0.5, 0.125, ((0, 32),))
    expert_down = gaussian(key_of[12], (EXPERTS, FFE, D), FFE ** -0.5, 0.25, ((0, 32),))
    routed_experts_keys = jax.random.split(jax.random.fold_in(key_of[13], 1), TOKEN_COUNT // TOK_DEV)
    routed_experts_turns = jax.random.permutation(jax.random.fold_in(key_of[13], 3), TOKEN_COUNT // TOK_DEV)
    routed_experts = jax.vmap(lambda own, number: assign_block(jax.random.fold_in(key_of[13], 2), own, number, TOK_DEV, EXPERTS, TOPK, CAP, 2))(routed_experts_keys, routed_experts_turns).reshape((TOKEN_COUNT, TOPK))
    route_weights = jnp.clip(jnp.exp(math.log(1.5) - 2.7080502 * jax.random.uniform(key_of[14], (TOKEN_COUNT, TOPK), jnp.float32) ** levels(key_of[14], (TOKEN_COUNT, TOPK), ((0, 32),), -0.2, 0.2)), 0.1, 1.5)
    return dict(queries=queries, key_heads=key_heads, value_heads=value_heads, head_gain=head_gain, residual=residual, out_weight=out_weight, norm_gain=norm_gain, shared_gate=shared_gate, shared_up=shared_up, shared_down=shared_down, expert_gate=expert_gate, expert_up=expert_up, expert_down=expert_down, routed_experts=routed_experts, route_weights=route_weights)


EPSILON = 1e-06

def block_terms(query_block, key_block, value_block, query_start, key_start):
    scale = 1.0 / math.sqrt(HEAD_DIM)
    scores = jnp.einsum('qhd,khd->hqk', query_block.astype(jnp.float32), key_block.astype(jnp.float32)) * scale
    query_places = query_start + lax.iota(jnp.int32, query_block.shape[0])
    key_places = key_start + lax.iota(jnp.int32, key_block.shape[0])
    earlier = (key_places[None, :] < query_places[:, None])[None]
    stay_log = jnp.where(earlier, jax.nn.log_sigmoid(-scores), 0.0)
    after_log = lax.cumsum(stay_log, axis=2, reverse=True) - stay_log
    weights = jnp.where(earlier, jnp.exp(jax.nn.log_sigmoid(scores) + after_log), 0.0).astype(jnp.bfloat16)
    partial_out = jnp.einsum('hqk,khd->qhd', weights.astype(jnp.float32), value_block.astype(jnp.float32))
    block_total = jnp.transpose(lax.optimization_barrier(jnp.sum(stay_log, axis=2)))
    return (block_total, partial_out)

def head_norm(mixed, head_gain):
    inverse = lax.rsqrt(lax.optimization_barrier(jnp.mean(mixed * mixed, axis=2, keepdims=True)) + EPSILON)
    normed = mixed * inverse * head_gain.reshape(mixed.shape[1], mixed.shape[2])
    return normed.reshape(mixed.shape[0], -1).astype(jnp.bfloat16)

def stick_breaking(queries, key_heads, value_heads):
    query_width = 512 if TOK_SP % 512 == 0 else TOK_SP
    query_all = queries.reshape(TOKEN_COUNT // query_width, query_width, HEADS, HEAD_DIM)
    key_all = key_heads.reshape(N_SP, TOK_SP, HEADS, HEAD_DIM)
    value_all = value_heads.reshape(N_SP, TOK_SP, HEADS, HEAD_DIM)

    def one_block(block_index):
        query_block = lax.dynamic_index_in_dim(query_all, block_index, 0, keepdims=False)
        query_start = block_index * query_width

        def one_shard(running, shard_index):
            key_start = shard_index * TOK_SP

            def compute(unused):
                key_block = lax.dynamic_index_in_dim(key_all, shard_index, 0, keepdims=False)
                value_block = lax.dynamic_index_in_dim(value_all, shard_index, 0, keepdims=False)
                return block_terms(query_block, key_block, value_block, query_start, key_start)

            def nothing(unused):
                return (jnp.zeros((query_width, HEADS), jnp.float32), jnp.zeros((query_width, HEADS, HEAD_DIM), jnp.float32))
            return (running, lax.cond(key_start < query_start + query_width, compute, nothing, 0))
        leftover, stacked = lax.scan(one_shard, jnp.int32(0), jnp.arange(N_SP, dtype=jnp.int32))
        totals, partials = stacked
        later = lax.cumsum(totals, axis=0, reverse=True) - totals
        return lax.optimization_barrier(jnp.sum(jnp.exp(later)[..., None] * partials, axis=0))
    mixed = lax.map(one_block, jnp.arange(TOKEN_COUNT // query_width, dtype=jnp.int32))
    return mixed.reshape(TOKEN_COUNT, HEADS, HEAD_DIM)

def expert_block(inputs):
    expert_rows, gate_weight, up_weight, down_weight = inputs
    gate_part = jnp.dot(expert_rows, gate_weight, preferred_element_type=jnp.float32)
    up_part = jnp.dot(expert_rows, up_weight, preferred_element_type=jnp.float32)
    hidden = (jax.nn.silu(gate_part) * up_part).astype(jnp.bfloat16)
    return jnp.dot(hidden, down_weight, preferred_element_type=jnp.float32).astype(jnp.bfloat16)

def routed_sum(expert_input, expert_gate, expert_up, expert_down, routed_experts, route_weights):
    device_count = N_SP * N_TP
    flat_experts = routed_experts.reshape(-1)
    expert_table = (flat_experts[:, None] == jnp.arange(EXPERTS, dtype=jnp.int32)[None, :]).astype(jnp.int32)
    expert_table = expert_table.reshape(device_count, TOK_DEV * TOPK, EXPERTS)
    ranking = (lax.optimization_barrier(jnp.sum(jnp.cumsum(expert_table, axis=1) * expert_table, axis=2)) - 1).reshape(-1)
    source = jnp.arange(TOKEN_COUNT * TOPK, dtype=jnp.int32) // (TOK_DEV * TOPK)
    slot_index = (flat_experts * device_count + source) * CAP + ranking
    repeated = jnp.repeat(expert_input, TOPK, axis=0)
    buffer = jnp.zeros((EXPERTS * device_count * CAP, D), jnp.bfloat16).at[slot_index].set(repeated)
    buffer = buffer.reshape(EXPERTS, device_count * CAP, D)
    results = lax.map(expert_block, (buffer, expert_gate, expert_up, expert_down)).reshape(-1, D)
    slot_grid = slot_index.reshape(TOKEN_COUNT, TOPK)
    routed = jnp.zeros((TOKEN_COUNT, D), jnp.float32)
    for choice_index in range(TOPK):
        picked = results[slot_grid[:, choice_index]].astype(jnp.float32)
        routed = routed + picked * route_weights[:, choice_index][:, None]
    return routed

def reference(queries, key_heads, value_heads, head_gain, residual, out_weight, norm_gain, shared_gate, shared_up, shared_down, expert_gate, expert_up, expert_down, routed_experts, route_weights):
    head_output = head_norm(stick_breaking(queries, key_heads, value_heads), head_gain)
    branch = jnp.dot(head_output, out_weight, preferred_element_type=jnp.float32)
    stream = (residual.astype(jnp.float32) + branch).astype(jnp.bfloat16)
    stream_wide = stream.astype(jnp.float32)
    inverse = lax.rsqrt(lax.optimization_barrier(jnp.mean(stream_wide * stream_wide, axis=1, keepdims=True)) + EPSILON)
    expert_input = (stream_wide * inverse * norm_gain).astype(jnp.bfloat16)
    shared_hidden = (jax.nn.silu(jnp.dot(expert_input, shared_gate, preferred_element_type=jnp.float32)) * jnp.dot(expert_input, shared_up, preferred_element_type=jnp.float32)).astype(jnp.bfloat16)
    shared_term = jnp.dot(shared_hidden, shared_down, preferred_element_type=jnp.float32)
    routed = routed_sum(expert_input, expert_gate, expert_up, expert_down, routed_experts, route_weights)
    return (stream_wide + shared_term + routed).astype(jnp.bfloat16)
```

```python
import functools
import math

import jax
import jax.numpy as jnp
from jax import lax
from jax.experimental import pallas as pl
from jax.experimental.pallas import tpu as pltpu
from jax.sharding import PartitionSpec as P

HEAD_DIM = 64
EPSILON = 1e-06
CHUNK = 256


def attention_step(*refs, step, inner, first, last):
    refs = list(refs)
    place_ref, query_ref, flag_ref, wide_flag_ref, gain_ref = refs[:5]
    block_refs = refs[5 : 5 + inner]
    refs = refs[5 + inner :]
    if not first:
        sum_in, later_in = refs[:2]
        refs = refs[2:]
    if last:
        out_ref, sum_ref, later_ref, held_ref = refs
    else:
        sum_ref, later_ref, held_ref = refs
    heads, rows, width = query_ref.shape
    tile = min(CHUNK, rows)
    tiles = rows // tile
    inner_place = place_ref[0]
    outer_place = place_ref[1]
    scale = math.log2(math.e) / math.sqrt(HEAD_DIM)
    if first:
        sum_ref[...] = jnp.zeros_like(sum_ref)
        later_ref[...] = jnp.zeros_like(later_ref)
    else:
        sum_ref[...] = sum_in[...]
        later_ref[...] = later_in[...]
    down = lax.broadcasted_iota(jnp.int32, (tile, tile), 0)
    across = lax.broadcasted_iota(jnp.int32, (tile, tile), 1)
    suffix = jnp.where(down > across, 1.0, 0.0).astype(jnp.bfloat16)

    def one_chunk(row_start, key_start, masked):
        query_rows = pl.ds(row_start, tile)
        key_rows = pl.ds(key_start, tile)
        keys = held_ref[key_rows, :width]
        values = held_ref[key_rows, width:]
        total = sum_ref[query_rows, :]
        for head in range(heads):
            scores = (
                lax.dot_general(
                    query_ref[head, query_rows, :],
                    keys,
                    (((1,), (1,)), ((), ())),
                    preferred_element_type=jnp.float32,
                )
                * scale
            )
            fold = jnp.log2(1.0 + jnp.exp2(-jnp.abs(scores)))
            stay = jnp.minimum(-scores, 0.0) - fold
            take = jnp.minimum(scores, 0.0) - fold
            if masked:
                earlier = across + key_start < down + row_start
                stay = jnp.where(earlier, stay, 0.0)
            high = stay.astype(jnp.bfloat16)
            low = (stay - high.astype(jnp.float32)).astype(jnp.bfloat16)
            after = jnp.dot(high, suffix, preferred_element_type=jnp.float32) + jnp.dot(
                low, suffix, preferred_element_type=jnp.float32
            )
            later = later_ref[head, query_rows, :]
            weights = jnp.exp2(take + after + jnp.concatenate([later] * (tile // 128), axis=1))
            if masked:
                weights = jnp.where(earlier, weights, 0.0)
            total = total + jnp.dot(
                weights.astype(jnp.bfloat16),
                values * flag_ref[head : head + 1, :],
                preferred_element_type=jnp.float32,
            )
            later_ref[head, query_rows, :] = later + jnp.sum(stay, axis=1, keepdims=True)
        sum_ref[query_rows, :] = total

    def walk(masked):
        def row_tile(row_index, unused):
            row_start = pl.multiple_of(row_index * tile, tile)

            def key_chunk(chunk_step, unused_too):
                key_index = (row_index if masked else tiles - 1) - chunk_step
                key_start = pl.multiple_of(key_index * tile, tile)
                one_chunk(row_start, key_start, masked)
                return 0

            if masked:
                one_chunk(row_start, row_start, True)

                def full_chunk(chunk_step, unused_too):
                    key_index = row_index - 1 - chunk_step
                    one_chunk(row_start, pl.multiple_of(key_index * tile, tile), False)
                    return 0

                lax.fori_loop(0, row_index, full_chunk, 0)
            else:
                lax.fori_loop(0, tiles, key_chunk, 0)
            return 0

        lax.fori_loop(0, tiles, row_tile, 0)

    def hold(key_place):
        for shift in range(inner):
            pl.when(lax.rem(inner_place - shift + inner, inner) == key_place)(
                functools.partial(copy_block, shift)
            )

    def copy_block(shift):
        held_ref[...] = block_refs[shift][...]

    if first:
        held_ref[...] = block_refs[0][...]
        walk(True)

    def one_block(block_step, unused):
        key_place = inner - 1 - block_step
        active = key_place < inner_place if first else outer_place >= step

        @pl.when(active)
        def _():
            hold(key_place)
            walk(False)

        return 0

    lax.fori_loop(0, inner, one_block, 0)

    if last:
        mixed = sum_ref[...]
        square = mixed * mixed
        inverse = jnp.zeros_like(mixed)
        for head in range(heads):
            flag = wide_flag_ref[head : head + 1, :]
            mean = jnp.sum(square * flag, axis=1, keepdims=True) * (1.0 / HEAD_DIM)
            inverse = inverse + lax.rsqrt(mean + EPSILON) * flag
        out_ref[...] = (mixed * inverse * gain_ref[...]).astype(jnp.bfloat16)


def stick_breaking(queries, key_heads, value_heads, head_gain):
    rows, width = queries.shape
    heads = width // HEAD_DIM
    shard_count = lax.axis_size("sp")
    shard_place = lax.axis_index("sp")
    inner = 1 << (int(math.log2(shard_count)) // 2)
    outer = shard_count // inner
    place = jnp.stack([shard_place % inner, shard_place // inner]).astype(jnp.int32)
    wide_flags = (
        jnp.arange(width, dtype=jnp.int32)[None, :] // HEAD_DIM
        == jnp.arange(heads, dtype=jnp.int32)[:, None]
    ).astype(jnp.float32)
    flags = wide_flags.astype(jnp.bfloat16)
    query_heads = queries[None] * flags[:, None, :]
    own = jnp.concatenate([key_heads, value_heads], axis=1)
    gain = head_gain[None, :]
    smem = pl.BlockSpec(memory_space=pltpu.SMEM)
    vmem = pl.BlockSpec(memory_space=pltpu.VMEM)
    arrived = [own]
    for step in range(1, outer):
        arrived.append(
            lax.ppermute(
                own, "sp", [(s, s + step * inner) for s in range(shard_count - step * inner)]
            )
        )
    state = ()
    for step in range(outer):
        blocks = [arrived[step]]
        for shift in range(1, inner):
            pairs = []
            for s in range(step * inner, shard_count):
                if step or s % inner + shift < inner:
                    pairs.append((s, s // inner * inner + (s % inner + shift) % inner))
            blocks.append(lax.ppermute(arrived[step], "sp", pairs))
        first, last = step == 0, step == outer - 1
        state_shapes = [
            jax.ShapeDtypeStruct((rows, width), jnp.float32),
            jax.ShapeDtypeStruct((heads, rows, 128), jnp.float32),
        ]
        scratch = [pltpu.VMEM((rows, 2 * width), jnp.bfloat16)]
        if last:
            out_shape = jax.ShapeDtypeStruct((rows, width), jnp.bfloat16)
            out_specs = vmem
            scratch = [pltpu.VMEM(s.shape, s.dtype) for s in state_shapes] + scratch
        else:
            out_shape = state_shapes
            out_specs = [vmem, vmem]
        state = pl.pallas_call(
            functools.partial(
                attention_step, step=step, inner=inner, first=first, last=last
            ),
            in_specs=[smem] + [vmem] * (4 + inner + len(state)),
            out_shape=out_shape,
            out_specs=out_specs,
            scratch_shapes=scratch,
            name="attention_step",
        )(place, query_heads, flags, wide_flags, gain, *blocks, *state)
    return state


def routed_sum(expert_input, expert_gate, expert_up, expert_down, routed_experts, route_weights):
    row_count, pick_count = routed_experts.shape
    local_experts = expert_gate.shape[0]
    model_width = expert_input.shape[1]
    sp_count = lax.axis_size("sp")
    tp_count = lax.axis_size("tp")
    device_count = sp_count * tp_count
    expert_count = local_experts * device_count
    capacity = max(2, 3 * row_count * pick_count // (2 * expert_count))
    flat_experts = routed_experts.reshape(-1)
    expert_table = (
        flat_experts[:, None] == jnp.arange(expert_count, dtype=jnp.int32)[None, :]
    ).astype(jnp.int32)
    ranking = jnp.sum(jnp.cumsum(expert_table, axis=0) * expert_table, axis=1) - 1
    holder = flat_experts // local_experts
    resident = flat_experts % local_experts
    slot_index = (resident * device_count + holder) * capacity + ranking
    placement = (
        slot_index[:, None] == jnp.arange(expert_count * capacity, dtype=jnp.int32)[None, :]
    ).astype(jnp.bfloat16)
    token_place = jnp.sum(placement.reshape(row_count, pick_count, -1), axis=1)
    outgoing = jnp.einsum(
        "rs,rd->sd", token_place, expert_input, preferred_element_type=jnp.float32
    ).astype(jnp.bfloat16)
    outgoing = outgoing.reshape(local_experts, device_count, capacity, model_width)
    arrived = lax.all_to_all(outgoing, ("sp", "tp"), split_axis=1, concat_axis=1, tiled=True)
    grouped = arrived.reshape(local_experts, -1, model_width)
    gate_part = jnp.einsum("erd,edf->erf", grouped, expert_gate, preferred_element_type=jnp.float32)
    up_part = jnp.einsum("erd,edf->erf", grouped, expert_up, preferred_element_type=jnp.float32)
    hidden = (jax.nn.silu(gate_part) * up_part).astype(jnp.bfloat16)
    result = jnp.einsum(
        "erf,efd->erd", hidden, expert_down, preferred_element_type=jnp.float32
    ).astype(jnp.bfloat16)
    returned = lax.all_to_all(
        result.reshape(arrived.shape), ("sp", "tp"), split_axis=1, concat_axis=1, tiled=True
    )
    gathered = jnp.dot(
        placement, returned.reshape(-1, model_width), preferred_element_type=jnp.float32
    )
    weighted = gathered.reshape(row_count, pick_count, model_width) * route_weights[:, :, None]
    return jnp.sum(weighted, axis=1)


def body(
    queries,
    key_heads,
    value_heads,
    head_gain,
    residual,
    out_weight,
    norm_gain,
    shared_gate,
    shared_up,
    shared_down,
    expert_gate,
    expert_up,
    expert_down,
    routed_experts,
    route_weights,
):
    head_output = stick_breaking(queries, key_heads, value_heads, head_gain)
    token_heads = lax.all_to_all(head_output, "tp", split_axis=0, concat_axis=1, tiled=True)
    branch = jnp.dot(token_heads, out_weight, preferred_element_type=jnp.float32)
    stream = (residual.astype(jnp.float32) + branch).astype(jnp.bfloat16)
    stream_wide = stream.astype(jnp.float32)
    inverse = lax.rsqrt(jnp.mean(stream_wide * stream_wide, axis=1, keepdims=True) + EPSILON)
    expert_input = (stream_wide * inverse * norm_gain).astype(jnp.bfloat16)
    shared_hidden = (
        jax.nn.silu(jnp.dot(expert_input, shared_gate, preferred_element_type=jnp.float32))
        * jnp.dot(expert_input, shared_up, preferred_element_type=jnp.float32)
    ).astype(jnp.bfloat16)
    shared_term = jnp.dot(shared_hidden, shared_down, preferred_element_type=jnp.float32)
    routed = routed_sum(
        expert_input, expert_gate, expert_up, expert_down, routed_experts, route_weights
    )
    return (stream_wide + shared_term + routed).astype(jnp.bfloat16)


def solution(mesh):
    return jax.shard_map(
        body,
        mesh=mesh,
        in_specs=(
            P("sp", "tp"),
            P("sp", "tp"),
            P("sp", "tp"),
            P("tp"),
            P(("sp", "tp"), None),
            P(),
            P(),
            P(),
            P(),
            P(),
            P(("sp", "tp"), None, None),
            P(("sp", "tp"), None, None),
            P(("sp", "tp"), None, None),
            P(("sp", "tp"), None),
            P(("sp", "tp"), None),
        ),
        out_specs=P(("sp", "tp"), None),
        check_vma=False,
    )
```

```python
import functools
import math

import jax
import jax.numpy as jnp
from jax import lax
from jax.experimental import pallas as pl
from jax.experimental.pallas import tpu as pltpu
from jax.sharding import PartitionSpec as P

HEAD_DIM = 64
EPSILON = 1e-06
CHUNK = 256


def attention_step(*refs, step, inner, first, last):
    refs = list(refs)
    place_ref, query_ref, flag_ref, wide_flag_ref, gain_ref = refs[:5]
    count = 1 if first else inner
    block_refs = refs[5 : 5 + count]
    refs = refs[5 + count :]
    if not first:
        sum_in, later_in = refs[:2]
        refs = refs[2:]
    if last:
        out_ref, sum_ref, later_ref, held_ref = refs
    else:
        sum_ref, later_ref, held_ref = refs
    heads, rows, width = query_ref.shape
    tile = min(CHUNK, rows)
    tiles = rows // tile
    inner_place = place_ref[0]
    outer_place = place_ref[1]
    scale = math.log2(math.e) / math.sqrt(HEAD_DIM)
    if first:
        sum_ref[...] = jnp.zeros_like(sum_ref)
        later_ref[...] = jnp.zeros_like(later_ref)
    else:
        sum_ref[...] = sum_in[...]
        later_ref[...] = later_in[...]
    down = lax.broadcasted_iota(jnp.int32, (tile, tile), 0)
    across = lax.broadcasted_iota(jnp.int32, (tile, tile), 1)
    suffix = jnp.where(down > across, 1.0, 0.0).astype(jnp.bfloat16)

    def one_chunk(row_start, key_start, masked):
        query_rows = pl.ds(row_start, tile)
        key_rows = pl.ds(key_start, tile)
        keys = held_ref[key_rows, :width]
        values = held_ref[key_rows, width:]
        total = sum_ref[query_rows, :]
        laters = [later_ref[head, query_rows, :] for head in range(heads)]
        all_scores = [
            lax.dot_general(
                query_ref[head, query_rows, :],
                keys,
                (((1,), (1,)), ((), ())),
                preferred_element_type=jnp.float32,
            )
            for head in range(heads)
        ]
        if masked:
            earlier = across + key_start < down + row_start
        takes, stays, afters = [], [], []
        for head in range(heads):
            scores = all_scores[head] * scale
            fold = jnp.log2(1.0 + jnp.exp2(-jnp.abs(scores)))
            stay = jnp.minimum(-scores, 0.0) - fold
            takes.append(jnp.minimum(scores, 0.0) - fold)
            if masked:
                stay = jnp.where(earlier, stay, 0.0)
            high = stay.astype(jnp.bfloat16)
            low = (stay - high.astype(jnp.float32)).astype(jnp.bfloat16)
            stays.append(stay)
            afters.append(
                jnp.dot(high, suffix, preferred_element_type=jnp.float32)
                + jnp.dot(low, suffix, preferred_element_type=jnp.float32)
            )
        for head in range(heads):
            later = jnp.concatenate([laters[head]] * (tile // 128), axis=1)
            weights = jnp.exp2(takes[head] + afters[head] + later)
            if masked:
                weights = jnp.where(earlier, weights, 0.0)
            total = total + jnp.dot(
                weights.astype(jnp.bfloat16),
                values * flag_ref[head : head + 1, :],
                preferred_element_type=jnp.float32,
            )
        for head in range(heads):
            later_ref[head, query_rows, :] = laters[head] + jnp.sum(
                stays[head], axis=1, keepdims=True
            )
        sum_ref[query_rows, :] = total

    def walk(masked):
        def row_tile(row_index, unused):
            row_start = pl.multiple_of(row_index * tile, tile)

            def key_chunk(chunk_step, unused_too):
                key_index = (row_index if masked else tiles - 1) - chunk_step
                key_start = pl.multiple_of(key_index * tile, tile)
                one_chunk(row_start, key_start, masked)
                return 0

            if masked:
                one_chunk(row_start, row_start, True)

                def full_chunk(chunk_step, unused_too):
                    key_index = row_index - 1 - chunk_step
                    one_chunk(row_start, pl.multiple_of(key_index * tile, tile), False)
                    return 0

                lax.fori_loop(0, row_index, full_chunk, 0)
            else:
                lax.fori_loop(0, tiles, key_chunk, 0)
            return 0

        lax.fori_loop(0, tiles, row_tile, 0)

    def hold(key_place):
        for shift in range(inner):
            pl.when(lax.rem(inner_place - shift + inner, inner) == key_place)(
                functools.partial(copy_block, shift)
            )

    def copy_block(shift):
        held_ref[...] = block_refs[shift][...]

    def one_block(block_step, unused):
        key_place = inner - 1 - block_step
        active = outer_place >= step if step else key_place < inner_place

        @pl.when(active)
        def _():
            hold(key_place)
            walk(False)

        return 0

    if first:
        held_ref[...] = block_refs[0][...]
        walk(True)
    else:
        lax.fori_loop(0, inner, one_block, 0)

    if last:
        mixed = sum_ref[...]
        square = mixed * mixed
        inverse = jnp.zeros_like(mixed)
        for head in range(heads):
            flag = wide_flag_ref[head : head + 1, :]
            mean = jnp.sum(square * flag, axis=1, keepdims=True) * (1.0 / HEAD_DIM)
            inverse = inverse + lax.rsqrt(mean + EPSILON) * flag
        out_ref[...] = (mixed * inverse * gain_ref[...]).astype(jnp.bfloat16)


def stick_breaking(queries, key_heads, value_heads, head_gain):
    rows, width = queries.shape
    heads = width // HEAD_DIM
    shard_count = lax.axis_size("sp")
    shard_place = lax.axis_index("sp")
    inner = 1 << (int(math.log2(shard_count)) // 2)
    outer = shard_count // inner
    place = jnp.stack([shard_place % inner, shard_place // inner]).astype(jnp.int32)
    wide_flags = (
        jnp.arange(width, dtype=jnp.int32)[None, :] // HEAD_DIM
        == jnp.arange(heads, dtype=jnp.int32)[:, None]
    ).astype(jnp.float32)
    flags = wide_flags.astype(jnp.bfloat16)
    query_heads = queries[None] * flags[:, None, :]
    own = jnp.concatenate([key_heads, value_heads], axis=1)
    gain = head_gain[None, :]
    smem = pl.BlockSpec(memory_space=pltpu.SMEM)
    vmem = pl.BlockSpec(memory_space=pltpu.VMEM)
    arrived = [own]
    for step in range(1, outer):
        arrived.append(
            lax.ppermute(
                own, "sp", [(s, s + step * inner) for s in range(shard_count - step * inner)]
            )
        )

    def exchange(block, step):
        blocks = [block]
        for shift in range(1, inner):
            pairs = []
            for s in range(step * inner, shard_count):
                if step or s % inner + shift < inner:
                    pairs.append((s, s // inner * inner + (s % inner + shift) % inner))
            blocks.append(lax.ppermute(block, "sp", pairs))
        return blocks

    def run(step, blocks, state, last=False):
        state_shapes = [
            jax.ShapeDtypeStruct((rows, width), jnp.float32),
            jax.ShapeDtypeStruct((heads, rows, 128), jnp.float32),
        ]
        scratch = [pltpu.VMEM((rows, 2 * width), jnp.bfloat16)]
        if last:
            out_shape = jax.ShapeDtypeStruct((rows, width), jnp.bfloat16)
            out_specs = vmem
            scratch = [pltpu.VMEM(s.shape, s.dtype) for s in state_shapes] + scratch
        else:
            out_shape = state_shapes
            out_specs = [vmem, vmem]
        return pl.pallas_call(
            functools.partial(
                attention_step, step=step, inner=inner, first=not state, last=last
            ),
            in_specs=[smem] + [vmem] * (4 + len(blocks) + len(state)),
            out_shape=out_shape,
            out_specs=out_specs,
            scratch_shapes=scratch,
            name="attention_step",
        )(place, query_heads, flags, wide_flags, gain, *blocks, *state)

    near = exchange(own, 0)
    state = run(0, [own], ())
    for step in range(outer):
        later_blocks = None
        if step + 1 < outer:
            block, state = lax.optimization_barrier((arrived[step + 1], tuple(state)))
            later_blocks = exchange(block, step + 1)
        state = run(step, near, state, last=step == outer - 1)
        near = later_blocks
    return state


def expert_step(mask_ref, rows_ref, gate_ref, up_ref, down_ref, out_ref, sum_ref):
    expert, piece = pl.program_id(0), pl.program_id(1)

    @pl.when((expert == 0) & (piece == 0))
    def _():
        sum_ref[...] = jnp.zeros_like(sum_ref)

    rows = rows_ref[...]
    gate = jnp.dot(rows, gate_ref[0], preferred_element_type=jnp.float32)
    up = jnp.dot(rows, up_ref[0], preferred_element_type=jnp.float32)
    owned = mask_ref[:, :1] == expert
    hidden = jnp.where(owned, gate / (1.0 + jnp.exp(-gate)) * up, 0.0).astype(jnp.bfloat16)
    sum_ref[...] += jnp.dot(hidden, down_ref[0], preferred_element_type=jnp.float32)

    @pl.when((expert == pl.num_programs(0) - 1) & (piece == pl.num_programs(1) - 1))
    def _():
        out_ref[...] = sum_ref[...].astype(jnp.bfloat16)


def run_experts(rows, resident, expert_gate, expert_up, expert_down):
    local_experts, model_width, hidden_width = expert_gate.shape
    row_count = rows.shape[0]
    piece = min(256, hidden_width)
    whole = lambda e, f: (0, 0)
    return pl.pallas_call(
        expert_step,
        grid=(local_experts, hidden_width // piece),
        in_specs=[
            pl.BlockSpec((row_count, 128), whole),
            pl.BlockSpec((row_count, model_width), whole),
            pl.BlockSpec((1, model_width, piece), lambda e, f: (e, 0, f)),
            pl.BlockSpec((1, model_width, piece), lambda e, f: (e, 0, f)),
            pl.BlockSpec((1, piece, model_width), lambda e, f: (e, f, 0)),
        ],
        out_shape=jax.ShapeDtypeStruct((row_count, model_width), jnp.bfloat16),
        out_specs=pl.BlockSpec((row_count, model_width), whole),
        scratch_shapes=[pltpu.VMEM((row_count, model_width), jnp.float32)],
        name="expert_step",
    )(resident, rows, expert_gate, expert_up, expert_down)


def routed_sum(expert_input, expert_gate, expert_up, expert_down, routed_experts, route_weights):
    row_count, pick_count = routed_experts.shape
    local_experts = expert_gate.shape[0]
    model_width = expert_input.shape[1]
    sp_count = lax.axis_size("sp")
    tp_count = lax.axis_size("tp")
    device_count = sp_count * tp_count
    expert_count = local_experts * device_count
    capacity = max(2, 3 * row_count * pick_count // (2 * expert_count))
    flat_experts = routed_experts.reshape(-1)
    expert_table = (
        flat_experts[:, None] == jnp.arange(expert_count, dtype=jnp.int32)[None, :]
    ).astype(jnp.int32)
    ranking = jnp.sum(jnp.cumsum(expert_table, axis=0) * expert_table, axis=1) - 1
    per_device = local_experts * capacity
    slot_index = flat_experts * capacity + ranking
    slots = jnp.arange(expert_count * capacity, dtype=jnp.int32)
    placement = slot_index.reshape(row_count, pick_count)[:, :, None] == slots[None, None, :]
    token_place = jnp.sum(placement.astype(jnp.bfloat16), axis=1)
    combine = jnp.sum(jnp.where(placement, route_weights[:, :, None], 0.0), axis=1)
    combine_high = lax.reduce_precision(combine, 8, 7)
    combine_low = (combine - combine_high).astype(jnp.bfloat16)
    combine_both = jnp.concatenate([combine_high.astype(jnp.bfloat16), combine_low], axis=0)
    outgoing = jnp.einsum(
        "rs,rd->sd", token_place, expert_input, preferred_element_type=jnp.float32
    ).astype(jnp.bfloat16)
    outgoing = outgoing.reshape(device_count, per_device, model_width)
    arrived = lax.all_to_all(outgoing, ("sp", "tp"), split_axis=0, concat_axis=0, tiled=True)
    owner = jnp.broadcast_to((slots % per_device // capacity)[:, None], (slots.shape[0], 128))
    result = run_experts(
        arrived.reshape(-1, model_width), owner, expert_gate, expert_up, expert_down
    )
    returned = lax.all_to_all(
        result.reshape(arrived.shape), ("sp", "tp"), split_axis=0, concat_axis=0, tiled=True
    )
    gathered = jnp.dot(
        combine_both, returned.reshape(-1, model_width), preferred_element_type=jnp.float32
    )
    return gathered[:row_count] + gathered[row_count:]


def body(
    queries,
    key_heads,
    value_heads,
    head_gain,
    residual,
    out_weight,
    norm_gain,
    shared_gate,
    shared_up,
    shared_down,
    expert_gate,
    expert_up,
    expert_down,
    routed_experts,
    route_weights,
):
    head_output = stick_breaking(queries, key_heads, value_heads, head_gain)
    token_heads = lax.all_to_all(head_output, "tp", split_axis=0, concat_axis=1, tiled=True)
    branch = jnp.dot(token_heads, out_weight, preferred_element_type=jnp.float32)
    stream = (residual.astype(jnp.float32) + branch).astype(jnp.bfloat16)
    stream_wide = stream.astype(jnp.float32)
    inverse = lax.rsqrt(jnp.mean(stream_wide * stream_wide, axis=1, keepdims=True) + EPSILON)
    expert_input = (stream_wide * inverse * norm_gain).astype(jnp.bfloat16)
    shared_hidden = (
        jax.nn.silu(jnp.dot(expert_input, shared_gate, preferred_element_type=jnp.float32))
        * jnp.dot(expert_input, shared_up, preferred_element_type=jnp.float32)
    ).astype(jnp.bfloat16)
    shared_term = jnp.dot(shared_hidden, shared_down, preferred_element_type=jnp.float32)
    routed = routed_sum(
        expert_input, expert_gate, expert_up, expert_down, routed_experts, route_weights
    )
    return (stream_wide + shared_term + routed).astype(jnp.bfloat16)


def solution(mesh):
    return jax.shard_map(
        body,
        mesh=mesh,
        in_specs=(
            P("sp", "tp"),
            P("sp", "tp"),
            P("sp", "tp"),
            P("tp"),
            P(("sp", "tp"), None),
            P(),
            P(),
            P(),
            P(),
            P(),
            P(("sp", "tp"), None, None),
            P(("sp", "tp"), None, None),
            P(("sp", "tp"), None, None),
            P(("sp", "tp"), None),
            P(("sp", "tp"), None),
        ),
        out_specs=P(("sp", "tp"), None),
        check_vma=False,
    )
```

```python
import functools
import math

import jax
import jax.numpy as jnp
import numpy as np
from jax import lax
from jax.experimental import pallas as pl
from jax.experimental.pallas import tpu as pltpu
from jax.sharding import PartitionSpec as P

HEAD_DIM = 64
EPSILON = 1e-06
CHUNK = 256


def attention_step(*refs, step, inner, first, last):
    refs = list(refs)
    place_ref, query_ref, flag_ref, wide_flag_ref, gain_ref = refs[:5]
    count = 1 if first else inner
    block_refs = refs[5 : 5 + count]
    refs = refs[5 + count :]
    if not first:
        sum_in, later_in = refs[:2]
        refs = refs[2:]
    if last:
        out_ref, sum_ref, later_ref, held_ref = refs
    else:
        sum_ref, later_ref, held_ref = refs
    heads, rows, width = query_ref.shape
    tile = min(CHUNK, rows)
    tiles = rows // tile
    inner_place = place_ref[0]
    outer_place = place_ref[1]
    scale = math.log2(math.e) / math.sqrt(HEAD_DIM)
    if first:
        sum_ref[...] = jnp.zeros_like(sum_ref)
        later_ref[...] = jnp.zeros_like(later_ref)
    else:
        sum_ref[...] = sum_in[...]
        later_ref[...] = later_in[...]
    down = lax.broadcasted_iota(jnp.int32, (tile, tile), 0)
    across = lax.broadcasted_iota(jnp.int32, (tile, tile), 1)
    suffix = jnp.where(down > across, 1.0, 0.0).astype(jnp.bfloat16)

    def one_chunk(row_start, key_start, masked):
        query_rows = pl.ds(row_start, tile)
        key_rows = pl.ds(key_start, tile)
        keys = held_ref[key_rows, :width]
        values = held_ref[key_rows, width:]
        total = sum_ref[query_rows, :]
        laters = [later_ref[head, query_rows, :] for head in range(heads)]
        all_scores = [
            lax.dot_general(
                query_ref[head, query_rows, :],
                keys,
                (((1,), (1,)), ((), ())),
                preferred_element_type=jnp.float32,
            )
            for head in range(heads)
        ]
        if masked:
            earlier = across + key_start < down + row_start
        takes, stays, afters = [], [], []
        for head in range(heads):
            scores = all_scores[head] * scale
            fold = jnp.log2(1.0 + jnp.exp2(-jnp.abs(scores)))
            stay = jnp.minimum(-scores, 0.0) - fold
            takes.append(jnp.minimum(scores, 0.0) - fold)
            if masked:
                stay = jnp.where(earlier, stay, 0.0)
            high = stay.astype(jnp.bfloat16)
            low = (stay - high.astype(jnp.float32)).astype(jnp.bfloat16)
            stays.append(stay)
            afters.append(
                jnp.dot(high, suffix, preferred_element_type=jnp.float32)
                + jnp.dot(low, suffix, preferred_element_type=jnp.float32)
            )
        for head in range(heads):
            later = jnp.concatenate([laters[head]] * (tile // 128), axis=1)
            weights = jnp.exp2(takes[head] + afters[head] + later)
            if masked:
                weights = jnp.where(earlier, weights, 0.0)
            total = total + jnp.dot(
                weights.astype(jnp.bfloat16),
                values * flag_ref[head : head + 1, :],
                preferred_element_type=jnp.float32,
            )
        for head in range(heads):
            later_ref[head, query_rows, :] = laters[head] + jnp.sum(
                stays[head], axis=1, keepdims=True
            )
        sum_ref[query_rows, :] = total

    def walk(masked):
        def row_tile(row_index, unused):
            row_start = pl.multiple_of(row_index * tile, tile)

            def key_chunk(chunk_step, unused_too):
                key_index = (row_index if masked else tiles - 1) - chunk_step
                key_start = pl.multiple_of(key_index * tile, tile)
                one_chunk(row_start, key_start, masked)
                return 0

            if masked:
                one_chunk(row_start, row_start, True)

                def full_chunk(chunk_step, unused_too):
                    key_index = row_index - 1 - chunk_step
                    one_chunk(row_start, pl.multiple_of(key_index * tile, tile), False)
                    return 0

                lax.fori_loop(0, row_index, full_chunk, 0)
            else:
                lax.fori_loop(0, tiles, key_chunk, 0)
            return 0

        lax.fori_loop(0, tiles, row_tile, 0)

    def hold(key_place):
        for shift in range(inner):
            pl.when(lax.rem(inner_place - shift + inner, inner) == key_place)(
                functools.partial(copy_block, shift)
            )

    def copy_block(shift):
        held_ref[...] = block_refs[shift][...]

    def one_block(block_step, unused):
        key_place = inner - 1 - block_step
        active = outer_place >= step if step else key_place < inner_place

        @pl.when(active)
        def _():
            hold(key_place)
            walk(False)

        return 0

    if first:
        held_ref[...] = block_refs[0][...]
        walk(True)
    else:
        lax.fori_loop(0, inner, one_block, 0)

    if last:
        mixed = sum_ref[...]
        square = mixed * mixed
        inverse = jnp.zeros_like(mixed)
        for head in range(heads):
            flag = wide_flag_ref[head : head + 1, :]
            mean = jnp.sum(square * flag, axis=1, keepdims=True) * (1.0 / HEAD_DIM)
            inverse = inverse + lax.rsqrt(mean + EPSILON) * flag
        out_ref[...] = (mixed * inverse * gain_ref[...]).astype(jnp.bfloat16)


def stick_breaking(queries, key_heads, value_heads, head_gain):
    rows, width = queries.shape
    heads = width // HEAD_DIM
    shard_count = lax.axis_size("sp")
    shard_place = lax.axis_index("sp")
    inner = 1 << (int(math.log2(shard_count)) // 2)
    outer = shard_count // inner
    place = jnp.stack([shard_place % inner, shard_place // inner]).astype(jnp.int32)
    wide_flags = (
        jnp.arange(width, dtype=jnp.int32)[None, :] // HEAD_DIM
        == jnp.arange(heads, dtype=jnp.int32)[:, None]
    ).astype(jnp.float32)
    flags = wide_flags.astype(jnp.bfloat16)
    query_heads = queries[None] * flags[:, None, :]
    own = jnp.concatenate([key_heads, value_heads], axis=1)
    gain = head_gain[None, :]
    smem = pl.BlockSpec(memory_space=pltpu.SMEM)
    vmem = pl.BlockSpec(memory_space=pltpu.VMEM)
    arrived = [own]
    for step in range(1, outer):
        arrived.append(
            lax.ppermute(
                own, "sp", [(s, s + step * inner) for s in range(shard_count - step * inner)]
            )
        )

    def exchange(block, step):
        blocks = [block]
        for shift in range(1, inner):
            pairs = []
            for s in range(step * inner, shard_count):
                if step or s % inner + shift < inner:
                    pairs.append((s, s // inner * inner + (s % inner + shift) % inner))
            blocks.append(lax.ppermute(block, "sp", pairs))
        return blocks

    def run(step, blocks, state, last=False):
        state_shapes = [
            jax.ShapeDtypeStruct((rows, width), jnp.float32),
            jax.ShapeDtypeStruct((heads, rows, 128), jnp.float32),
        ]
        scratch = [pltpu.VMEM((rows, 2 * width), jnp.bfloat16)]
        if last:
            out_shape = jax.ShapeDtypeStruct((rows, width), jnp.bfloat16)
            out_specs = vmem
            scratch = [pltpu.VMEM(s.shape, s.dtype) for s in state_shapes] + scratch
        else:
            out_shape = state_shapes
            out_specs = [vmem, vmem]
        return pl.pallas_call(
            functools.partial(
                attention_step, step=step, inner=inner, first=not state, last=last
            ),
            in_specs=[smem] + [vmem] * (4 + len(blocks) + len(state)),
            out_shape=out_shape,
            out_specs=out_specs,
            scratch_shapes=scratch,
            name="attention_step",
        )(place, query_heads, flags, wide_flags, gain, *blocks, *state)

    near = exchange(own, 0)
    state = run(0, [own], ())
    for step in range(outer):
        later_blocks = None
        if step + 1 < outer:
            block, state = lax.optimization_barrier((arrived[step + 1], tuple(state)))
            later_blocks = exchange(block, step + 1)
        state = run(step, near, state, last=step == outer - 1)
        near = later_blocks
    return state


def expert_step(
    mask_ref, rows_ref, gate_ref, up_ref, down_ref, out_ref, hidden_ref, *, pieces, wide_steps
):
    step = pl.program_id(0)
    piece = gate_ref.shape[2]

    @pl.when(step < wide_steps)
    def _():
        rows = rows_ref[...]
        gate = jnp.dot(rows, gate_ref[0], preferred_element_type=jnp.float32)
        up = jnp.dot(rows, up_ref[0], preferred_element_type=jnp.float32)
        owned = mask_ref[:, :1] == step // pieces
        hidden = jnp.where(owned, gate / (1.0 + jnp.exp(-gate)) * up, 0.0)
        columns = pl.ds(pl.multiple_of(step * piece, piece), piece)
        hidden_ref[:, columns] = hidden.astype(jnp.bfloat16)

    @pl.when(step >= wide_steps)
    def _():
        out_ref[...] = jnp.dot(
            hidden_ref[...], down_ref[...], preferred_element_type=jnp.float32
        ).astype(jnp.bfloat16)


def run_experts(rows, resident, expert_gate, expert_up, expert_down):
    local_experts, model_width, hidden_width = expert_gate.shape
    row_count = rows.shape[0]
    piece = min(256, hidden_width)
    pieces = hidden_width // piece
    wide_steps = local_experts * pieces
    out_piece = min(512, model_width)
    whole = lambda i: (0, 0)

    def wide(i):
        j = jnp.minimum(i, wide_steps - 1)
        return (j // pieces, 0, j % pieces)

    narrow = lambda i: (0, jnp.maximum(i - wide_steps, 0))
    return pl.pallas_call(
        functools.partial(expert_step, pieces=pieces, wide_steps=wide_steps),
        grid=(wide_steps + model_width // out_piece,),
        in_specs=[
            pl.BlockSpec((row_count, 128), whole),
            pl.BlockSpec((row_count, model_width), whole),
            pl.BlockSpec((1, model_width, piece), wide),
            pl.BlockSpec((1, model_width, piece), wide),
            pl.BlockSpec((local_experts * hidden_width, out_piece), narrow),
        ],
        out_shape=jax.ShapeDtypeStruct((row_count, model_width), jnp.bfloat16),
        out_specs=pl.BlockSpec((row_count, out_piece), narrow),
        scratch_shapes=[pltpu.VMEM((row_count, local_experts * hidden_width), jnp.bfloat16)],
        name="expert_step",
    )(resident, rows, expert_gate, expert_up, expert_down.reshape(-1, model_width))


def combine_step(combine_ref, returned_ref, base_ref, out_ref):
    rows = base_ref.shape[0]
    both = jnp.dot(combine_ref[...], returned_ref[...], preferred_element_type=jnp.float32)
    out_ref[...] = (base_ref[...] + (both[:rows] + both[rows:])).astype(jnp.bfloat16)


def run_combine(combine, returned, base):
    rows, model_width = base.shape
    piece = min(512, model_width)
    column = lambda i: (0, i)
    return pl.pallas_call(
        combine_step,
        grid=(model_width // piece,),
        in_specs=[
            pl.BlockSpec(combine.shape, lambda i: (0, 0)),
            pl.BlockSpec((returned.shape[0], piece), column),
            pl.BlockSpec((rows, piece), column),
        ],
        out_shape=jax.ShapeDtypeStruct((rows, model_width), jnp.bfloat16),
        out_specs=pl.BlockSpec((rows, piece), column),
        name="combine_step",
    )(combine, returned, base)


def add_routed(
    base, expert_input, expert_gate, expert_up, expert_down, routed_experts, route_weights
):
    row_count, pick_count = routed_experts.shape
    local_experts = expert_gate.shape[0]
    model_width = expert_input.shape[1]
    sp_count = lax.axis_size("sp")
    tp_count = lax.axis_size("tp")
    device_count = sp_count * tp_count
    expert_count = local_experts * device_count
    capacity = max(2, 3 * row_count * pick_count // (2 * expert_count))
    flat_experts = routed_experts.reshape(-1)
    expert_table = (
        flat_experts[:, None] == jnp.arange(expert_count, dtype=jnp.int32)[None, :]
    ).astype(jnp.int32)
    ranking = jnp.sum(jnp.cumsum(expert_table, axis=0) * expert_table, axis=1) - 1
    per_device = local_experts * capacity
    slot_index = flat_experts * capacity + ranking
    slots = jnp.arange(expert_count * capacity, dtype=jnp.int32)
    placement = slot_index.reshape(row_count, pick_count)[:, :, None] == slots[None, None, :]
    token_place = jnp.sum(placement.astype(jnp.bfloat16), axis=1)
    combine = jnp.sum(jnp.where(placement, route_weights[:, :, None], 0.0), axis=1)
    combine_high = lax.reduce_precision(combine, 8, 7)
    combine_low = (combine - combine_high).astype(jnp.bfloat16)
    combine_both = jnp.concatenate([combine_high.astype(jnp.bfloat16), combine_low], axis=0)
    outgoing = jnp.einsum(
        "rs,rd->sd", token_place, expert_input, preferred_element_type=jnp.float32
    ).astype(jnp.bfloat16)
    outgoing = outgoing.reshape(device_count, per_device, model_width)
    arrived = lax.all_to_all(outgoing, ("sp", "tp"), split_axis=0, concat_axis=0, tiled=True)
    slot_owner = np.arange(expert_count * capacity, dtype=np.int32) % per_device // capacity
    owner = jnp.asarray(np.repeat(slot_owner[:, None], 128, axis=1))
    result = run_experts(
        arrived.reshape(-1, model_width), owner, expert_gate, expert_up, expert_down
    )
    returned = lax.all_to_all(
        result.reshape(arrived.shape), ("sp", "tp"), split_axis=0, concat_axis=0, tiled=True
    )
    return run_combine(combine_both, returned.reshape(-1, model_width), base)


def body(
    queries,
    key_heads,
    value_heads,
    head_gain,
    residual,
    out_weight,
    norm_gain,
    shared_gate,
    shared_up,
    shared_down,
    expert_gate,
    expert_up,
    expert_down,
    routed_experts,
    route_weights,
):
    head_output = stick_breaking(queries, key_heads, value_heads, head_gain)
    token_heads = lax.all_to_all(head_output, "tp", split_axis=0, concat_axis=1, tiled=True)
    branch = jnp.dot(token_heads, out_weight, preferred_element_type=jnp.float32)
    stream = (residual.astype(jnp.float32) + branch).astype(jnp.bfloat16)
    stream_wide = stream.astype(jnp.float32)
    inverse = lax.rsqrt(jnp.mean(stream_wide * stream_wide, axis=1, keepdims=True) + EPSILON)
    expert_input = (stream_wide * inverse * norm_gain).astype(jnp.bfloat16)
    shared_hidden = (
        jax.nn.silu(jnp.dot(expert_input, shared_gate, preferred_element_type=jnp.float32))
        * jnp.dot(expert_input, shared_up, preferred_element_type=jnp.float32)
    ).astype(jnp.bfloat16)
    shared_term = jnp.dot(shared_hidden, shared_down, preferred_element_type=jnp.float32)
    return add_routed(
        stream_wide + shared_term,
        expert_input,
        expert_gate,
        expert_up,
        expert_down,
        routed_experts,
        route_weights,
    )


def solution(mesh):
    return jax.shard_map(
        body,
        mesh=mesh,
        in_specs=(
            P("sp", "tp"),
            P("sp", "tp"),
            P("sp", "tp"),
            P("tp"),
            P(("sp", "tp"), None),
            P(),
            P(),
            P(),
            P(),
            P(),
            P(("sp", "tp"), None, None),
            P(("sp", "tp"), None, None),
            P(("sp", "tp"), None, None),
            P(("sp", "tp"), None),
            P(("sp", "tp"), None),
        ),
        out_specs=P(("sp", "tp"), None),
        check_vma=False,
    )
```
